32 devices in a mesh: grp: 2 (over y), sp: 4 (over z), tp: 4 (over x, core).
Axes of the slice: x: 2, y: 2, z: 4, core: 2. Of those that a mesh axis runs over, the one named last changes fastest.
Arguments:
- tokens_in: bfloat16 [2048, 2048], P(('grp', 'sp')), parts along dimension 0, may hold values from -6 to 6
- input_gain: float32 [2048], replicated, may hold values from 0.1 to 1.9
- w_query: bfloat16 [2048, 1024], P('sp', 'tp'), may hold values from -0.125 to 0.125
- w_key: bfloat16 [2048, 1024], P('sp', 'tp'), may hold values from -1 to 1
- w_value: bfloat16 [2048, 1024], P('sp', 'tp'), may hold values from -0.125 to 0.125
- w_gates: bfloat16 [2048, 32], P('sp', 'tp'), may hold values from -3 to 3
- w_glu_value: bfloat16 [2048, 1024], P('sp', 'tp'), may hold values from -0.125 to 0.125
- sigmoid_opener_matrix: bfloat16 [2048, 1024], P('sp', 'tp'), may hold values from -0.125 to 0.125
- log_decay: float32 [2048, 16], P(('grp', 'sp'), 'tp'), parts along dimension 0, may hold values from -1 to 0
- head_gain: float32 [128], replicated, may hold values from 0.1 to 1.9
- conv_kernel: float32 [31, 1024], P(None, 'tp'), may hold values from -12 to 12
- norm_gain: float32 [1024], P('tp'), may hold values from 0.1 to 1.9
- norm_shift: float32 [1024], P('tp'), may hold values from -3 to 3
- out_delta: bfloat16 [2048, 1024], P(None, 'tp'), may hold values from -0.125 to 0.125
- out_conv: bfloat16 [2048, 1024], P(None, 'tp'), may hold values from -0.125 to 0.125
Outputs:
- mixed: bfloat16 [2048, 2048], P(('grp', 'sp'), 'tp'), parts along dimension 0
The draws below stay inside these ranges and needn't reach their ends.
There are 2 independent parts, one for each index of `grp`. The reference program is written for one: setup_inputs(seed, part) draws one part's arguments, and reference() takes and returns one part's arrays. A program takes and returns all parts, laid end to end along the dimension named above; an argument that names none is the same for every part. Nothing has to cross between parts.
All inputs are finite; a program needn't handle non-finite values.
Results may differ from the reference program's by a relative error of at most 0.015.
Values may be sent and summed in bfloat16 or wider, within the bound.
No kernel may reach another device: no remote copies, remote signals or barrier semaphores. Data moves between devices by JAX's collectives and lax.ppermute only.
A program may use at most 64 MiB of HBM per device.

```python
import jax
import jax.numpy as jnp
from jax import lax

D = 2048
HEADS = 8
HEAD_DIM = 128
CONV_CH = 1024
KERNEL = 31
BLOCK = 64
TOK_DEV = 256
SEQ = 1024
A_W = 1024
N_TP = 4


def draw_log_decay(key, part):
    streams = jax.random.split(jax.random.fold_in(key, 11), 6)
    columns = 2 * HEADS
    fast_share = 0.5
    picker = jax.random.uniform(streams[0], (columns,), jnp.float32)
    fast_rate = jax.random.uniform(streams[1], (columns,), jnp.float32, 0.015, 0.04)
    slow_rate = jax.random.uniform(streams[2], (columns,), jnp.float32, 0.04, 0.16) / SEQ
    forgetting_pace = jnp.where(picker < fast_share, fast_rate, slow_rate)
    multiplier_amount = jnp.exp(jax.random.uniform(streams[3], (SEQ // TOK_DEV, columns), jnp.float32, 0.0, 1.0986))
    multiplier_amount = jnp.repeat(multiplier_amount, TOK_DEV, axis=0)
    spots = jax.random.randint(streams[4], (2, columns), 0, SEQ)
    places = jnp.arange(SEQ)[:, None]
    masked_elements = (places == spots[0][None, :]) | (places == spots[1][None, :])
    objective_readings = jax.random.uniform(streams[5], (SEQ, columns), jnp.float32, 0.2, 0.35)
    clustered_bunches = jnp.where(masked_elements, jnp.log(1.0 - objective_readings), 0.0)
    return (-(forgetting_pace[None, :] * multiplier_amount) + clustered_bunches).astype(jnp.float32)


def draw_conv_kernel(key, part):
    streams = jax.random.split(jax.random.fold_in(key, 23), 2)
    channel_slot = jnp.arange(CONV_CH).astype(jnp.float32)
    random_perturbation = jax.random.uniform(streams[1], (CONV_CH,), jnp.float32)
    entries = jnp.clip(jax.random.normal(streams[0], (KERNEL, CONV_CH), jnp.float32), -4.0, 4.0)
    reach = 10.0
    scale = reach ** ((channel_slot + random_perturbation) / CONV_CH)
    return (entries * scale[None, :] / jnp.sqrt(float(KERNEL))).astype(jnp.float32)


def unit_entries(stream, shape):
    return jnp.clip(jax.random.normal(stream, shape, jnp.float32), -4.0, 4.0)


def draw_w_key(key, part):
    streams = jax.random.split(jax.random.fold_in(key, 31), 2)
    strong_count = HEAD_DIM * 3 // 8
    weak_energy = 0.356 * (HEAD_DIM - strong_count)
    ratio_square = max(1.0, (0.04 * SEQ - weak_energy) / (0.5 * strong_count))
    orders = jax.vmap(lambda sub_key: jax.random.permutation(sub_key, HEAD_DIM))(jax.random.split(streams[0], HEADS))
    column_scale = jnp.where(orders < strong_count, ratio_square ** 0.5, 1.0).reshape(HEADS * HEAD_DIM).astype(jnp.float32)
    entries = unit_entries(streams[1], (D, HEADS * HEAD_DIM))
    return (entries * column_scale[None, :] / jnp.sqrt(float(D))).astype(jnp.bfloat16)


def draw_w_gates(key, part):
    stream = jax.random.fold_in(key, 37)
    roles = jnp.arange(4 * HEADS) % 4
    column_scale = jnp.where((roles == 1) | (roles == 3), 4.0, 1.0).astype(jnp.float32)
    entries = unit_entries(stream, (D, 4 * HEADS))
    return (entries * column_scale[None, :] / jnp.sqrt(float(D))).astype(jnp.bfloat16)


def shard_levels(key, extent, shards, smallest, top_value):
    level = 1.0
    for axis_at, parts in shards:
        heights = jax.random.uniform(jax.random.fold_in(jax.random.fold_in(key, 6), axis_at), (parts,), jnp.float32, smallest / len(shards), top_value / len(shards))
        level = level * jnp.repeat(jnp.exp(heights), extent[axis_at] // parts).reshape((-1,) + (1,) * (len(extent) - 1 - axis_at))
    return level


def bell_draw(rng, dims, scale, most, cuts=(), kind=jnp.bfloat16):
    array = jax.random.normal(rng, dims, jnp.float32) * scale
    if len(cuts) > 0:
        array = shard_levels(rng, dims, cuts, -0.22, 0.18) * array
    return jnp.clip(array, min=-most, max=most).astype(kind)


def setup_inputs(seed: int = 0, part: int = 0) -> dict:
    key_list = jax.random.split(jax.random.key(seed), 16)
    part_keys = jax.random.split(jax.random.fold_in(key_list[15], part), 16)
    tokens_in = bell_draw(part_keys[0], (SEQ, D), 1.0, 6.0, ((0, 4),))
    input_gain = jnp.clip(1.0 + 0.18 * jax.random.normal(key_list[1], (D,), jnp.float32), 0.1, 1.9)
    w_query = bell_draw(key_list[2], (D, A_W), D ** -0.5, 0.125, ((0, 4), (1, 4)))
    w_key = draw_w_key(jax.random.fold_in(key_list[15], 71), part)
    w_value = bell_draw(key_list[4], (D, A_W), D ** -0.5, 0.125, ((0, 4), (1, 4)))
    w_gates = draw_w_gates(jax.random.fold_in(key_list[15], 71), part)
    w_glu_value = bell_draw(key_list[6], (D, CONV_CH), D ** -0.5, 0.125, ((0, 4), (1, 4)))
    sigmoid_opener_matrix = bell_draw(key_list[7], (D, CONV_CH), D ** -0.5, 0.125, ((0, 4), (1, 4)))
    log_decay = draw_log_decay(jax.random.fold_in(jax.random.fold_in(key_list[15], part), 71), part)
    head_gain = jnp.clip(1.0 + 0.18 * jax.random.normal(key_list[9], (HEAD_DIM,), jnp.float32), 0.1, 1.9)
    conv_kernel = draw_conv_kernel(jax.random.fold_in(key_list[15], 71), part)
    norm_gain = jnp.clip(1.0 + 0.18 * jax.random.normal(key_list[11], (CONV_CH,), jnp.float32), 0.1, 1.9)
    norm_shift = bell_draw(key_list[12], (CONV_CH,), 0.5, 3.0, ((0, 4),), jnp.float32)
    out_delta = bell_draw(key_list[13], (D, A_W), (A_W + CONV_CH) ** -0.5, 0.125, ((1, 4),))
    out_conv = bell_draw(key_list[14], (D, CONV_CH), (A_W + CONV_CH) ** -0.5, 0.125, ((1, 4),))
    return {"tokens_in": tokens_in, "input_gain": input_gain, "w_query": w_query, "w_key": w_key, "w_value": w_value, "w_gates": w_gates, "w_glu_value": w_glu_value, "sigmoid_opener_matrix": sigmoid_opener_matrix, "log_decay": log_decay, "head_gain": head_gain, "conv_kernel": conv_kernel, "norm_gain": norm_gain, "norm_shift": norm_shift, "out_delta": out_delta, "out_conv": out_conv}


PRECISE = lax.Precision.HIGHEST
EPSILON = 1e-06
BETA_SHIFT = 6.0

def high_dot(left, right):
    return jnp.matmul(left, right, precision=PRECISE)

def swap_last(tensor):
    return jnp.swapaxes(tensor, -1, -2)

def block_terms(query, key_rows, values, decay_log, beta_rate, block):
    head_count, length = (query.shape[0], query.shape[1])
    blocks = length // block

    def to_blocks(tensor):
        return tensor.reshape((head_count, blocks, block) + tensor.shape[2:])
    query, key_rows, values, decay_log, beta_rate = (to_blocks(tensor) for tensor in (query, key_rows, values, decay_log, beta_rate))
    cumulative = jnp.cumsum(decay_log, axis=-1)
    positions = jnp.arange(block)
    on_or_below = positions[:, None] >= positions[None, :]
    strict = positions[:, None] > positions[None, :]
    log_gaps = cumulative[..., :, None] - cumulative[..., None, :]
    weighting = jnp.where(on_or_below, jnp.exp(jnp.where(on_or_below, log_gaps, 0.0)), 0.0)
    scaled_keys = key_rows * beta_rate[..., None]
    lower_part = jnp.where(strict, high_dot(scaled_keys, swap_last(key_rows)) * weighting, 0.0)
    identity = jnp.eye(block, dtype=jnp.float32)
    inverse = jax.scipy.linalg.solve_triangular(identity + lower_part, jnp.broadcast_to(identity, lower_part.shape), lower=True, unit_diagonal=True)
    update = high_dot(inverse, values * beta_rate[..., None])
    mixed_keys = high_dot(inverse, scaled_keys * jnp.exp(cumulative)[..., None])
    in_block = jnp.where(on_or_below, high_dot(query, swap_last(key_rows)) * weighting, 0.0)
    q_decayed = query * jnp.exp(cumulative)[..., None]
    k_decayed = key_rows * jnp.exp(cumulative[..., -1:] - cumulative)[..., None]
    end_decay = jnp.exp(cumulative[..., -1])
    return tuple((jnp.moveaxis(tensor, 1, 0) for tensor in (update, mixed_keys, in_block, q_decayed, k_decayed, end_decay)))

def delta_scan(query, key_rows, values, decay_log, beta_rate):
    stacked = block_terms(query, key_rows, values, decay_log, beta_rate, BLOCK)
    head_count, length, head_width = query.shape

    def advance(state_now, pieces):
        update, mixed_keys, in_block, q_decayed, k_decayed, end_decay = pieces
        new_values = update - high_dot(mixed_keys, state_now)
        output = high_dot(q_decayed, state_now) + high_dot(in_block, new_values)
        state_now = state_now * end_decay[:, None, None] + high_dot(swap_last(k_decayed), new_values)
        return (state_now, output)
    zero_state = jnp.zeros((head_count, head_width, values.shape[2]), jnp.float32)
    _, output = lax.scan(advance, zero_state, stacked)
    return jnp.moveaxis(output, 0, 1).reshape(head_count, length, values.shape[2])

def reference(tokens_in, input_gain, w_query, w_key, w_value, w_gates, w_glu_value, sigmoid_opener_matrix, log_decay, head_gain, conv_kernel, norm_gain, norm_shift, out_delta, out_conv):
    rows = tokens_in.astype(jnp.float32)
    normed = (rows * lax.rsqrt(lax.optimization_barrier(jnp.mean(rows * rows, axis=-1, keepdims=True)) + EPSILON) * input_gain).astype(jnp.bfloat16)

    def project(weight):
        return jnp.dot(normed.astype(jnp.float32), weight.astype(jnp.float32), preferred_element_type=jnp.float32)

    def by_head(tensor):
        return jnp.swapaxes(jax.nn.silu(tensor).reshape(SEQ, HEADS, HEAD_DIM), 0, 1)

    def unit_rows(tensor):
        return tensor * lax.rsqrt(lax.optimization_barrier(jnp.sum(tensor * tensor, axis=-1, keepdims=True)) + EPSILON)
    query = unit_rows(by_head(project(w_query))) * HEAD_DIM ** (-0.5)
    key_rows = unit_rows(by_head(project(w_key)))
    values = by_head(project(w_value))
    gate_parts = project(w_gates).reshape(SEQ, HEADS, 4)
    rate_parts = log_decay.reshape(SEQ, HEADS, 2)
    decay_fore = jnp.swapaxes(rate_parts[:, :, 0] * (0.5 + jax.nn.sigmoid(gate_parts[:, :, 0])), 0, 1)
    beta_fore = jnp.swapaxes(jax.nn.sigmoid(gate_parts[:, :, 1] - BETA_SHIFT), 0, 1)
    decay_back = jnp.swapaxes(rate_parts[:, :, 1] * (0.5 + jax.nn.sigmoid(gate_parts[:, :, 2])), 0, 1)
    beta_back = jnp.swapaxes(jax.nn.sigmoid(gate_parts[:, :, 3] - BETA_SHIFT), 0, 1)

    def reversed_rows(tensor):
        return jnp.flip(tensor, axis=1)
    fore = delta_scan(query, key_rows, values, decay_fore, beta_fore)
    back = reversed_rows(delta_scan(reversed_rows(query), reversed_rows(key_rows), reversed_rows(values), reversed_rows(decay_back), reversed_rows(beta_back)))
    joined = fore + back
    joined = joined * lax.rsqrt(lax.optimization_barrier(jnp.mean(joined * joined, axis=-1, keepdims=True)) + EPSILON) * head_gain
    delta_mix = jnp.swapaxes(joined, 0, 1).reshape(SEQ, HEADS * HEAD_DIM).astype(jnp.bfloat16)
    glu_rows = (project(w_glu_value) * jax.nn.sigmoid(project(sigmoid_opener_matrix))).astype(jnp.bfloat16)
    half_width = KERNEL // 2
    padded = jnp.pad(glu_rows.astype(jnp.float32), ((half_width, half_width), (0, 0)))
    conv_rows = padded[0:SEQ] * conv_kernel[0]
    for offset in range(1, KERNEL):
        conv_rows = conv_rows + padded[offset:offset + SEQ] * conv_kernel[offset]
    center = lax.optimization_barrier(jnp.mean(conv_rows, axis=-1))
    spread = lax.optimization_barrier(jnp.mean(conv_rows * conv_rows, axis=-1)) - center * center
    normal_rows = (conv_rows - center[:, None]) * lax.rsqrt(spread + EPSILON)[:, None]
    filtered_blend = jax.nn.silu(normal_rows * norm_gain + norm_shift).astype(jnp.bfloat16)
    head_cols = HEADS * HEAD_DIM // N_TP
    channel_columns = CONV_CH // N_TP
    result = jnp.zeros((SEQ, D), jnp.float32)
    for group in range(N_TP):
        partial_sum = jnp.dot(delta_mix[:, group * head_cols:(group + 1) * head_cols].astype(jnp.float32), out_delta[:, group * head_cols:(group + 1) * head_cols].T.astype(jnp.float32), preferred_element_type=jnp.float32)
        partial_sum = partial_sum + jnp.dot(filtered_blend[:, group * channel_columns:(group + 1) * channel_columns].astype(jnp.float32), out_conv[:, group * channel_columns:(group + 1) * channel_columns].T.astype(jnp.float32), preferred_element_type=jnp.float32)
        rounded = lax.optimization_barrier(partial_sum.astype(jnp.bfloat16))
        result = result + rounded.astype(jnp.float32)
    return result.astype(jnp.bfloat16)
```

```python
import functools

import jax
import jax.numpy as jnp
from jax import lax
from jax.experimental import pallas as pl
from jax.experimental.pallas import tpu as pltpu
from jax.sharding import PartitionSpec as P

CONV_CH = 1024
BLOCK = 64


PRECISE = lax.Precision.HIGHEST
EPSILON = 1e-06
BETA_SHIFT = 6.0


def entering(value, axis, combine, identity, reverse):
    devices, place = (lax.axis_size(axis), lax.axis_index(axis))
    everything = jax.tree.map(
        lambda part, kind: lax.all_gather(part.astype(kind), axis),
        value,
        (jnp.bfloat16, jnp.bfloat16),
    )
    start = jax.tree.map(
        lambda part, zero: jnp.broadcast_to(jnp.asarray(zero, part.dtype), part.shape),
        value,
        identity,
    )

    def lap(k, before):
        at = devices - 1 - k if reverse else k
        reached = at > place if reverse else at < place
        new = combine(
            before, jax.tree.map(lambda part, own: part[at].astype(own.dtype), everything, value)
        )
        return jax.tree.map(lambda a, b: jnp.where(reached, a, b), new, before)

    return lax.fori_loop(0, devices, lap, start)


def with_halo(block, sides, width):
    for axis, dim in sides:
        count = lax.axis_size(axis)
        forward = [(i, i + 1) for i in range(count - 1)]
        backward = [(target, source) for source, target in forward]
        low = lax.ppermute(
            lax.slice_in_dim(block, block.shape[dim] - width, None, axis=dim), axis, forward
        )
        high = lax.ppermute(lax.slice_in_dim(block, 0, width, axis=dim), axis, backward)
        block = jnp.concatenate([low, block, high], axis=dim)
    return block


def high_dot(left, right):
    return jnp.matmul(left, right, precision=PRECISE)


def swap_last(tensor):
    return jnp.swapaxes(tensor, -1, -2)


def block_terms(query, key_rows, values, decay_log, beta_rate, block):
    head_count, length = (query.shape[0], query.shape[1])
    blocks = length // block

    def to_blocks(tensor):
        return tensor.reshape((head_count, blocks, block) + tensor.shape[2:])

    query, key_rows, values, decay_log, beta_rate = (
        to_blocks(tensor) for tensor in (query, key_rows, values, decay_log, beta_rate)
    )
    cumulative = jnp.cumsum(decay_log, axis=-1)
    positions = jnp.arange(block)
    on_or_below = positions[:, None] >= positions[None, :]
    strict = positions[:, None] > positions[None, :]
    log_gaps = cumulative[..., :, None] - cumulative[..., None, :]
    weighting = jnp.where(on_or_below, jnp.exp(jnp.where(on_or_below, log_gaps, 0.0)), 0.0)
    scaled_keys = key_rows * beta_rate[..., None]
    lower_part = jnp.where(strict, high_dot(scaled_keys, swap_last(key_rows)) * weighting, 0.0)
    identity = jnp.eye(block, dtype=jnp.float32)
    inverse = jax.scipy.linalg.solve_triangular(
        identity + lower_part,
        jnp.broadcast_to(identity, lower_part.shape),
        lower=True,
        unit_diagonal=True,
    )
    update = high_dot(inverse, values * beta_rate[..., None])
    mixed_keys = high_dot(inverse, scaled_keys * jnp.exp(cumulative)[..., None])
    in_block = jnp.where(on_or_below, high_dot(query, swap_last(key_rows)) * weighting, 0.0)
    q_decayed = query * jnp.exp(cumulative)[..., None]
    k_decayed = key_rows * jnp.exp(cumulative[..., -1:] - cumulative)[..., None]
    end_decay = jnp.exp(cumulative[..., -1])
    return tuple(
        (
            jnp.moveaxis(tensor, 1, 0)
            for tensor in (update, mixed_keys, in_block, q_decayed, k_decayed, end_decay)
        )
    )


def delta_local(query, key_rows, values, decay_log, beta_rate):
    stacked = block_terms(query, key_rows, values, decay_log, beta_rate, BLOCK)
    head_count, length, head_width = query.shape
    identity = jnp.broadcast_to(
        jnp.eye(head_width, dtype=jnp.float32), (head_count, head_width, head_width)
    )
    zero_state = jnp.zeros((head_count, head_width, values.shape[2]), jnp.float32)

    def advance(carry, pieces):
        state_now, carried = carry
        update, mixed_keys, in_block, q_decayed, k_decayed, end_decay = pieces
        new_values = update - high_dot(mixed_keys, state_now)
        output = high_dot(q_decayed, state_now) + high_dot(in_block, new_values)
        reading = high_dot(q_decayed - high_dot(in_block, mixed_keys), carried)
        passing = end_decay[:, None, None] * identity - high_dot(swap_last(k_decayed), mixed_keys)
        state_now = state_now * end_decay[:, None, None] + high_dot(
            swap_last(k_decayed), new_values
        )
        return ((state_now, high_dot(passing, carried)), (output, reading))

    (state_now, carried), (output, reading) = lax.scan(advance, (zero_state, identity), stacked)
    output = jnp.moveaxis(output, 0, 1).reshape(head_count, length, values.shape[2])
    reading = jnp.moveaxis(reading, 0, 1).reshape(head_count, length, head_width)
    return (output, reading, carried, state_now)


def chain(earlier, later):
    return (high_dot(later[0], earlier[0]), high_dot(later[0], earlier[1]) + later[1])


def reversed_rows(tensor):
    return jnp.flip(tensor, axis=1)


def delta_branch(query_proj, key_proj, value_proj, gate_proj, log_decay, head_gain):
    head_width = head_gain.shape[0]
    length = query_proj.shape[0]
    head_count = query_proj.shape[1] // head_width

    def by_head(tensor):
        return jnp.swapaxes(jax.nn.silu(tensor).reshape(length, head_count, head_width), 0, 1)

    def unit_rows(tensor):
        return tensor * lax.rsqrt(jnp.sum(tensor * tensor, axis=-1, keepdims=True) + EPSILON)

    query = unit_rows(by_head(query_proj)) * head_width ** (-0.5)
    key_rows = unit_rows(by_head(key_proj))
    values = by_head(value_proj)
    gate_parts = gate_proj.reshape(length, head_count, 4)
    rate_parts = log_decay.reshape(length, head_count, 2)
    decay_fore = jnp.swapaxes(
        rate_parts[:, :, 0] * (0.5 + jax.nn.sigmoid(gate_parts[:, :, 0])), 0, 1
    )
    beta_fore = jnp.swapaxes(jax.nn.sigmoid(gate_parts[:, :, 1] - BETA_SHIFT), 0, 1)
    decay_back = jnp.swapaxes(
        rate_parts[:, :, 1] * (0.5 + jax.nn.sigmoid(gate_parts[:, :, 2])), 0, 1
    )
    beta_back = jnp.swapaxes(jax.nn.sigmoid(gate_parts[:, :, 3] - BETA_SHIFT), 0, 1)
    identity = jnp.broadcast_to(
        jnp.eye(head_width, dtype=jnp.float32), (head_count, head_width, head_width)
    )
    zero_state = jnp.zeros((head_count, head_width, head_width), jnp.float32)
    forward_out, forward_read, forward_map, forward_end = delta_local(
        query, key_rows, values, decay_fore, beta_fore
    )
    forward_start = entering(
        (forward_map, forward_end), "sp", chain, (identity, zero_state), False
    )[1]
    back_out, back_read, back_map, back_end = delta_local(
        reversed_rows(query),
        reversed_rows(key_rows),
        reversed_rows(values),
        reversed_rows(decay_back),
        reversed_rows(beta_back),
    )
    back_start = entering((back_map, back_end), "sp", chain, (identity, zero_state), True)[1]
    joined = forward_out + high_dot(forward_read, forward_start)
    joined = joined + reversed_rows(back_out + high_dot(back_read, back_start))
    joined = (
        joined * lax.rsqrt(jnp.mean(joined * joined, axis=-1, keepdims=True) + EPSILON) * head_gain
    )
    return jnp.swapaxes(joined, 0, 1).reshape(length, head_count * head_width).astype(jnp.bfloat16)


def conv_branch(value_proj, gate_proj, conv_kernel, norm_gain, norm_shift):
    glu_rows = (value_proj * jax.nn.sigmoid(gate_proj)).astype(jnp.bfloat16)
    half_width = conv_kernel.shape[0] // 2
    length = glu_rows.shape[0]
    padded = with_halo(glu_rows, (("sp", 0),), half_width).astype(jnp.float32)
    conv_rows = padded[0:length] * conv_kernel[0]
    for offset in range(1, conv_kernel.shape[0]):
        conv_rows = conv_rows + padded[offset : offset + length] * conv_kernel[offset]
    row_sum, row_squares = lax.psum(
        (jnp.sum(conv_rows, axis=-1), jnp.sum(conv_rows * conv_rows, axis=-1)), "tp"
    )
    center = row_sum / CONV_CH
    spread = row_squares / CONV_CH - center * center
    normal_rows = (conv_rows - center[:, None]) * lax.rsqrt(spread + EPSILON)[:, None]
    return jax.nn.silu(normal_rows * norm_gain + norm_shift).astype(jnp.bfloat16)


def on_device(
    tokens_in,
    input_gain,
    w_query,
    w_key,
    w_value,
    w_gates,
    w_glu_value,
    sigmoid_opener_matrix,
    log_decay,
    head_gain,
    conv_kernel,
    norm_gain,
    norm_shift,
    out_delta,
    out_conv,
):
    rows = tokens_in.astype(jnp.float32)
    normed = (
        rows * lax.rsqrt(jnp.mean(rows * rows, axis=-1, keepdims=True) + EPSILON) * input_gain
    ).astype(jnp.bfloat16)
    weight_rows = (
        lax.all_gather(w_query, "sp", axis=0, tiled=True),
        lax.all_gather(w_key, "sp", axis=0, tiled=True),
        lax.all_gather(w_value, "sp", axis=0, tiled=True),
        lax.all_gather(w_gates, "sp", axis=0, tiled=True),
        lax.all_gather(w_glu_value, "sp", axis=0, tiled=True),
        lax.all_gather(sigmoid_opener_matrix, "sp", axis=0, tiled=True),
    )
    projected = tuple(
        (
            jnp.dot(normed, rows_here, preferred_element_type=jnp.float32)
            for rows_here in weight_rows
        )
    )
    delta_mix = delta_branch(
        projected[0], projected[1], projected[2], projected[3], log_decay, head_gain
    )
    filtered_blend = conv_branch(projected[4], projected[5], conv_kernel, norm_gain, norm_shift)
    contract = (((1,), (1,)), ((), ()))
    term = lax.dot_general(delta_mix, out_delta, contract, preferred_element_type=jnp.float32)
    term = term + lax.dot_general(
        filtered_blend, out_conv, contract, preferred_element_type=jnp.float32
    )
    return lax.psum_scatter(term.astype(jnp.bfloat16), "tp", scatter_dimension=1, tiled=True)


NT = (((1,), (1,)), ((), ()))
NN = (((1,), (0,)), ((), ()))
TN = (((0,), (0,)), ((), ()))
BASE = 16
VMEM_SPEC = pl.BlockSpec(memory_space=pltpu.VMEM)


def mxu(left, right, dims=NN):
    return lax.dot_general(
        left.astype(jnp.bfloat16),
        right.astype(jnp.bfloat16),
        dims,
        preferred_element_type=jnp.float32,
    )


def halves(value):
    high = value.astype(jnp.bfloat16)
    return high, (value - high.astype(jnp.float32)).astype(jnp.bfloat16)


def mxu_fine(left, right, dims=NN):
    left_high, left_low = halves(left)
    right_high, right_low = halves(right)
    return (
        mxu(left_high, right_high, dims)
        + mxu(left_high, right_low, dims)
        + mxu(left_low, right_high, dims)
    )


def call(kernel, out_shape, args, flops=1e8, scratch=(), name=None):
    return pl.pallas_call(
        kernel,
        out_shape=out_shape,
        in_specs=[VMEM_SPEC] * len(args),
        out_specs=jax.tree.map(lambda _: VMEM_SPEC, out_shape),
        scratch_shapes=list(scratch),
        cost_estimate=pl.CostEstimate(
            flops=int(flops), bytes_accessed=1 << 20, transcendentals=0
        ),
        name=name,
    )(*args)


def norm_kernel(tokens, near, far, gain, normed):
    place, core = lax.axis_index("sp") % 2, lax.axis_index("tp") % 2
    rows, width = tokens.shape
    part = near.shape[1]
    step = 16

    @pl.loop(0, rows // step)
    def _(i):
        here = pl.ds(pl.multiple_of(i * step, step), step)
        own = tokens[here, :].astype(jnp.float32)
        scale = lax.rsqrt(jnp.mean(own * own, axis=-1, keepdims=True) + EPSILON)
        at = pl.ds(pl.multiple_of(place * rows + i * step, step), step)
        normed[at, :] = (own * scale * gain[...]).astype(jnp.bfloat16)
        a, b = near[here, :].astype(jnp.float32), far[here, :].astype(jnp.float32)
        total = jnp.sum(a * a, axis=-1, keepdims=True) + jnp.sum(b * b, axis=-1, keepdims=True)
        scale = lax.rsqrt(total / width + EPSILON)
        at = pl.ds(pl.multiple_of((1 - place) * rows + i * step, step), step)
        for value, which in ((a, core), (b, 1 - core)):
            columns = pl.ds(pl.multiple_of(which * part, part), part)
            normed[at, columns] = (value * scale * gain[:, columns]).astype(jnp.bfloat16)


def columns_of(normed, shard, half, depth):
    return normed[:, pl.ds(pl.multiple_of((shard * 2 + half) * depth, depth), depth)]


def project(normed, own, crossed, swapped, pick):
    count = len(crossed) + 1
    me, copy = lax.axis_index("sp"), lax.axis_index("grp")
    depth = pick(own).shape[0] // 2
    whole = normed[:, pl.ds(pl.multiple_of(me * 2 * depth, 2 * depth), 2 * depth)]
    total = mxu(whole, pick(own))
    for k in range(1, count):
        shard = lax.rem(me - k + count, count)
        for half, pieces in ((copy, crossed), (1 - copy, swapped)):
            total = total + mxu(
                columns_of(normed, shard, half, depth), pieces[k - 1][0:depth, :]
            )
    return total


def substitution(coupling, size, lower):
    row = lax.broadcasted_iota(jnp.int32, (size, size), 0)
    lane = lax.broadcasted_iota(jnp.int32, (size, size), 1)
    same = (row // BASE) == (lane // BASE)
    diagonal = jnp.where(same, coupling, 0.0)
    packed = diagonal[0:BASE, :]
    for k in range(1, size // BASE):
        packed = packed + diagonal[k * BASE : (k + 1) * BASE, :]
    tall = jnp.concatenate([packed] * BASE, axis=0)
    slot = lax.broadcasted_iota(jnp.int32, (BASE * BASE, size), 0) // BASE
    column = lax.broadcasted_iota(jnp.int32, (BASE * BASE, size), 1) % BASE
    tall = jnp.where(slot == column, tall, 0.0)
    ones = jnp.where(same, 1.0, 0.0).astype(jnp.bfloat16)
    high, low = halves(tall)
    lowest = (tall - high.astype(jnp.float32) - low.astype(jnp.float32)).astype(jnp.bfloat16)
    spread = mxu(high, ones) + mxu(low, ones) + mxu(lowest, ones)
    small_row = lax.broadcasted_iota(jnp.int32, (BASE, size), 0)
    small_lane = lax.broadcasted_iota(jnp.int32, (BASE, size), 1) % BASE
    solved = jnp.where(small_row == small_lane, 1.0, 0.0)
    order = range(BASE - 1) if lower else range(BASE - 1, 0, -1)
    for j in order:
        solved = solved - spread[j * BASE : (j + 1) * BASE, :] * solved[j : j + 1, :]
    return jnp.where(same, jnp.concatenate([solved] * (size // BASE), axis=0), 0.0)


def inverse_of(coupling, size, lower):
    found = substitution(coupling, size, lower)
    row = lax.broadcasted_iota(jnp.int32, (size, size), 0)
    lane = lax.broadcasted_iota(jnp.int32, (size, size), 1)
    width = BASE
    while width < size:
        up, left = row // width, lane // width
        beside = (up // 2 == left // 2) & ((up > left) if lower else (up < left))
        link = jnp.where(beside, coupling, 0.0)
        found = found - mxu_fine(found, mxu_fine(link, found))
        width *= 2
    return found


def unit_rows_of(value):
    return value * lax.rsqrt(jnp.sum(value * value, axis=-1, keepdims=True) + EPSILON)


def silu(value):
    return value * jax.nn.sigmoid(value)


def delta_kernel(others, *refs):
    normed, w_query, w_key, w_value, gates_own, rates_own, rates_near = refs[:7]
    crossed, swapped = refs[7 : 7 + others], refs[7 + others : 7 + 2 * others]
    out, reading, state, gate_rows, rate_rows, table = refs[7 + 2 * others :]
    me, copy = lax.axis_index("sp"), lax.axis_index("grp")
    count = others + 1
    place, late = me % 2, me // 2
    depth = w_query.shape[0] // 2
    head = w_query.shape[1] // 2
    size = rates_own.shape[1]
    mine = pl.ds(pl.multiple_of(place * head, head), head)

    def pick(own):
        return jnp.concatenate([w[:, mine] for w in own], axis=1)

    projected = project(normed, (w_query, w_key, w_value), crossed, swapped, pick)
    whole = normed[:, pl.ds(pl.multiple_of(me * 2 * depth, 2 * depth), 2 * depth)]
    gates = mxu(gates_own[...], whole, NT)
    for k in range(1, count):
        shard = lax.rem(me - k + count, count)
        for half, pieces in ((copy, crossed), (1 - copy, swapped)):
            gates = gates + mxu(
                pieces[k - 1][depth : depth + 16, 0:depth],
                columns_of(normed, shard, half, depth),
                NT,
            )
    gate_rows[...] = gates
    for block in range(2):
        at = slice(block * size, (block + 1) * size)
        rate_rows[:, at] = jnp.where(place == block, rates_own[...], rates_near[...])

    query = unit_rows_of(silu(projected[:, 0:head])) * head ** (-0.5)
    keys = unit_rows_of(silu(projected[:, head : 2 * head]))
    values = silu(projected[:, 2 * head : 3 * head])

    row = lax.broadcasted_iota(jnp.int32, (size, size), 0)
    lane = lax.broadcasted_iota(jnp.int32, (size, size), 1)
    table[...] = jnp.zeros_like(table)
    for d in range(2):
        decay = rate_rows[pl.ds(2 * place + d, 1), :] * (
            0.5 + jax.nn.sigmoid(gate_rows[pl.ds(4 * place + 2 * d, 1), :])
        )
        rate = jax.nn.sigmoid(gate_rows[pl.ds(4 * place + 2 * d + 1, 1), :] - BETA_SHIFT)
        summing = (row <= lane) if d == 0 else (row >= lane)
        summing = jnp.where(summing, 1.0, 0.0).astype(jnp.bfloat16)
        high, low = halves(decay)
        lowest = (decay - high.astype(jnp.float32) - low.astype(jnp.float32)).astype(jnp.bfloat16)
        for block in range(2):
            at = slice(block * size, (block + 1) * size)
            table[d : d + 1, at] = sum(
                mxu(jnp.broadcast_to(part[:, at], (8, size)), summing)[0:1, :]
                for part in (high, low, lowest)
            )
        table[2 + d : 3 + d, :] = rate
    upright = table[...].T

    solved = []
    for block in range(2):
        at = slice(block * size, (block + 1) * size)
        k, q, v = keys[at], query[at], values[at]
        alike = mxu_fine(k, k, NT)
        asked = mxu(q, k, NT)
        for d in range(2):
            lower = d == 0
            sums, sums_row = upright[at, d : d + 1], table[d : d + 1, at]
            rate = upright[at, 2 + d : 3 + d]
            reach = (row >= lane) if lower else (row <= lane)
            weight = jnp.where(reach, jnp.exp(jnp.where(reach, sums - sums_row, 0.0)), 0.0)
            coupling = jnp.where(row == lane, 0.0, alike * weight) * rate
            decayed = jnp.exp(sums)
            inverse = inverse_of(coupling, size, lower)
            wanted = mxu(inverse, jnp.concatenate([v * rate, k * (rate * decayed)], axis=1))
            seen = mxu(asked * weight, wanted)
            last = sums[size - 1 : size] if lower else sums[0:1]
            pushed = mxu(k * jnp.exp(last - sums), wanted, TN)
            end_decay = jnp.exp(last)
            solved.append(
                (
                    seen[:, 0:head],
                    q * decayed - seen[:, head:],
                    pushed[:, 0:head],
                    pushed[:, head:],
                    end_decay,
                )
            )
    results = []
    for d in range(2):
        first, second = (solved[d], solved[2 + d]) if d == 0 else (solved[2 + d], solved[d])
        carried = first[2]
        later_out = second[0] + mxu(second[1], carried)
        end = second[2] + second[4] * carried - mxu(second[3], carried)
        reads = mxu(second[1], first[3])
        later_read = first[4] * second[1] - reads
        outs, reads = [first[0], later_out], [first[1], later_read]
        if d == 1:
            outs, reads = outs[::-1], reads[::-1]
        results.append((outs, reads, end))
    (fore, fore_read, fore_end), (back, back_read, back_end) = results
    for block in range(2):
        at = slice(block * size, (block + 1) * size)
        out[at, :] = fore[block] + back[block]
        reading[at, :] = jnp.where(late == 1, fore_read[block], back_read[block]).astype(
            jnp.bfloat16
        )
    state[...] = jnp.where(late == 0, fore_end, back_end).astype(jnp.bfloat16)


def mix_kernel(local, reading, state, gain, keep, give, whole):
    place = lax.axis_index("sp") % 2
    size = local.shape[0] // 2
    joined = local[...] + mxu(reading[...], state[...])
    scale = lax.rsqrt(jnp.mean(joined * joined, axis=-1, keepdims=True) + EPSILON)
    whole[...] = joined * scale * gain[...]
    keep[...] = whole[pl.ds(pl.multiple_of(place * size, size), size), :].astype(jnp.bfloat16)
    give[...] = whole[pl.ds(pl.multiple_of((1 - place) * size, size), size), :].astype(
        jnp.bfloat16
    )


def glu_kernel(others, *refs):
    normed, w_value, w_gate = refs[:3]
    crossed, swapped = refs[3 : 3 + others], refs[3 + others : 3 + 2 * others]
    keep, give, edge_same, edge_other, rows = refs[3 + 2 * others :]
    place = lax.axis_index("sp") % 2
    width = w_value.shape[1] // 2
    mine = pl.ds(pl.multiple_of(place * width, width), width)

    def pick(own):
        return jnp.concatenate([w[:, mine] for w in own], axis=1)

    projected = project(normed, (w_value, w_gate), crossed, swapped, pick)
    rows[...] = projected[:, 0:width] * jax.nn.sigmoid(projected[:, width:])
    halo = edge_same.shape[0]
    size = keep.shape[0] - halo

    def cut(start, length):
        return rows[pl.ds(pl.multiple_of(start, halo), length), :].astype(jnp.bfloat16)

    keep[...] = cut(place * (size - halo), size + halo)
    give[...] = cut((1 - place) * (size - halo), size + halo)
    edge_same[...] = cut((1 - place) * (2 * size - halo), halo)
    edge_other[...] = cut(place * (2 * size - halo), halo)


def conv_kernel_body(main_same, main_other, edge_same, edge_other, taps, rows, sums, wide):
    place = lax.axis_index("sp") % 2
    halo = edge_same.shape[0]
    size = main_same.shape[0] - halo
    width = main_same.shape[1]
    count = taps.shape[0]
    for main, edge, which in (
        (main_same, edge_same, place),
        (main_other, edge_other, 1 - place),
    ):
        columns = pl.ds(pl.multiple_of(which * width, width), width)
        at = pl.ds(pl.multiple_of((1 - place) * halo, halo), size + halo)
        wide[at, columns] = main[...].astype(jnp.float32)
        at = pl.ds(pl.multiple_of(place * (size + halo), halo), halo)
        wide[at, columns] = edge[...].astype(jnp.float32)
    step = 32
    for start in range(0, size, step):
        total = jnp.zeros((step, 2 * width), jnp.float32)
        for j in range(count):
            offset = start + halo + j - count // 2
            total = total + wide[offset : offset + step, :] * taps[j : j + 1, :]
        rows[start : start + step, :] = total
    total = rows[...]
    lane = lax.broadcasted_iota(jnp.int32, (size, 128), 1)
    sums_tall = jnp.where(
        lane == 0,
        jnp.sum(total, axis=-1, keepdims=True),
        jnp.where(lane == 1, jnp.sum(total * total, axis=-1, keepdims=True), 0.0),
    )
    sums[...] = sums_tall.T[0:8, :]


def conv_mix_kernel(channels, rows, sums, gain, shift, mixed):
    size = rows.shape[0]
    tall = jnp.concatenate([sums[...], jnp.zeros((120, size), jnp.float32)], axis=0).T
    center = tall[:, 0:1] / channels
    spread = tall[:, 1:2] / channels - center * center
    normal = (rows[...] - center) * lax.rsqrt(spread + EPSILON)
    mixed[...] = silu(normal * gain[...] + shift[...]).astype(jnp.bfloat16)


def out_kernel(delta_keep, delta_take, conv_mix, w_delta, w_conv, keep, give, terms):
    place, core = lax.axis_index("sp") % 2, lax.axis_index("tp") % 2
    same, take = delta_keep[...], delta_take[...]
    first = jnp.where(place == 0, same, take)
    second = jnp.where(place == 0, take, same)
    left = jnp.concatenate([first, second, conv_mix[...]], axis=1)
    piece = w_delta.shape[0] // 4
    for x in range(2):
        for which, target in ((core, keep), (1 - core, give)):
            at = pl.ds(pl.multiple_of((2 * x + which) * piece, piece), piece)
            right = jnp.concatenate([w_delta[at, :], w_conv[at, :]], axis=1)
            target[:, x * piece : (x + 1) * piece] = mxu(left, right, NT).astype(target.dtype)


def swap(value, axis, distance):
    count = lax.axis_size(axis)
    return lax.ppermute(value, axis, [(i, i ^ distance) for i in range(count)])


def shifted(value, axis, k):
    count = lax.axis_size(axis)
    return lax.ppermute(value, axis, [(i, (i + k) % count) for i in range(count)])


def paired(
    tokens_in,
    input_gain,
    w_query,
    w_key,
    w_value,
    w_gates,
    w_glu_value,
    sigmoid_opener_matrix,
    log_decay,
    head_gain,
    conv_kernel,
    norm_gain,
    norm_shift,
    out_delta,
    out_conv,
):
    count = lax.axis_size("sp")
    me, copy, tp = lax.axis_index("sp"), lax.axis_index("grp"), lax.axis_index("tp")
    place = me % 2
    rows, width = tokens_in.shape
    head = head_gain.shape[0]
    depth = w_query.shape[0] // 2
    bf16, f32 = jnp.bfloat16, jnp.float32
    shape = jax.ShapeDtypeStruct
    half_channels = w_glu_value.shape[1] // 2

    gates_tall = jnp.pad(w_gates.T, ((0, 16 - w_gates.shape[1]), (0, 0)))
    gates_half = lax.dynamic_slice(gates_tall, (0, copy * depth), (16, depth))
    gates_half = jnp.pad(gates_half, ((0, 0), (0, 3 * head - depth)))

    def message(weights, parity, piece, extra=None):
        parts = [lax.dynamic_slice(w, (copy * depth, parity * piece), (depth, piece)) for w in weights]
        whole = jnp.concatenate(parts, axis=1)
        return whole if extra is None else jnp.concatenate([whole, extra], axis=0)

    delta_weights = (w_query, w_key, w_value)
    glu_weights = (w_glu_value, sigmoid_opener_matrix)
    delta_messages = [message(delta_weights, p, head, gates_half) for p in (place, 1 - place)]
    glu_messages = [message(glu_weights, p, half_channels) for p in (place, 1 - place)]
    hops = sorted(range(1, count), key=lambda k: (k % 2, k))

    crossed, swapped = {}, {}
    for k in hops:
        crossed[k] = shifted(delta_messages[k % 2], "sp", k)
    part = width // 2
    near = swap(lax.dynamic_slice(tokens_in, (0, (tp % 2) * part), (rows, part)), "sp", 1)
    rates = jnp.pad(log_decay.T, ((0, 8 - log_decay.shape[1]), (0, 0)))
    rates_near = swap(rates, "sp", 1)
    for k in hops:
        swapped[k] = swap(crossed[k], "grp", 1)
    far = swap(near, "tp", 1)
    glu_crossed = {k: shifted(glu_messages[k % 2], "sp", k) for k in hops}
    glu_swapped = {k: swap(glu_crossed[k], "grp", 1) for k in hops}

    normed = call(
        norm_kernel,
        shape((2 * rows, width), bf16),
        (tokens_in, near, far, input_gain[None, :]),
        flops=3e9,
        name="norm",
    )
    order = range(1, count)
    local, reading, state = call(
        functools.partial(delta_kernel, count - 1),
        (shape((2 * rows, head), f32), shape((2 * rows, head), bf16), shape((head, head), bf16)),
        (normed, w_query, w_key, w_value, gates_tall, rates, rates_near)
        + tuple(crossed[k] for k in order)
        + tuple(swapped[k] for k in order),
        flops=1e10,
        scratch=(
            pltpu.VMEM((16, 2 * rows), f32),
            pltpu.VMEM((8, 2 * rows), f32),
            pltpu.VMEM((128, 2 * rows), f32),
        ),
        name="delta",
    )
    state_in = swap(state, "sp", 2)
    halo = 16
    keep, give, edge_same, edge_other = call(
        functools.partial(glu_kernel, count - 1),
        (shape((rows + halo, half_channels), bf16),) * 2 + (shape((halo, half_channels), bf16),) * 2,
        (normed, w_glu_value, sigmoid_opener_matrix)
        + tuple(glu_crossed[k] for k in order)
        + tuple(glu_swapped[k] for k in order),
        flops=2e9,
        scratch=(pltpu.VMEM((2 * rows, half_channels), f32),),
        name="glu",
    )
    taken = swap(give, "sp", 1)
    outer_same = [(i, i + 2 if i % 2 == 0 else i - 2) for i in range(count)]
    outer_other = [(i, i - 1 if i % 2 == 0 else i + 1) for i in range(count)]
    inside = lambda pairs: [(a, b) for a, b in pairs if 0 <= b < count]
    edge_same = lax.ppermute(edge_same, "sp", inside(outer_same))
    edge_other = lax.ppermute(edge_other, "sp", inside(outer_other))
    channels = 2 * half_channels
    conv_rows, sums = call(
        conv_kernel_body,
        (shape((rows, channels), f32), shape((8, rows), f32)),
        (keep, taken, edge_same, edge_other, conv_kernel),
        flops=2e9,
        scratch=(pltpu.VMEM((rows + 2 * halo, channels), f32),),
        name="conv",
    )
    sums = lax.psum(sums, "tp")
    conv_mix = call(
        functools.partial(conv_mix_kernel, channels * lax.axis_size("tp")),
        shape((rows, channels), bf16),
        (conv_rows, sums, norm_gain[None, :], norm_shift[None, :]),
        flops=1e9,
        name="conv_mix",
    )
    delta_keep, delta_give = call(
        mix_kernel,
        (shape((rows, head), bf16),) * 2,
        (local, reading, state_in, head_gain[None, :]),
        flops=1e9,
        scratch=(pltpu.VMEM((2 * rows, head), f32),),
        name="mix",
    )
    delta_take = swap(delta_give, "sp", 1)
    features = out_delta.shape[0]
    keep, give = call(
        out_kernel,
        (shape((rows, features // 2), f32), shape((rows, features // 2), bf16)),
        (delta_keep, delta_take, conv_mix, out_delta, out_conv),
        flops=2e9,
        scratch=(pltpu.VMEM((8, 128), f32),),
        name="out",
    )
    both = keep + swap(give, "tp", 1).astype(f32)
    piece = features // 4
    x = tp // 2
    own = lax.dynamic_slice(both, (0, x * piece), (rows, piece))
    other = lax.dynamic_slice(both, (0, (1 - x) * piece), (rows, piece)).astype(bf16)
    return (own + swap(other, "tp", 2).astype(f32)).astype(bf16)


def solution(mesh):
    sizes = mesh.shape

    def step(*arguments):
        tokens_in, w_query, head_gain, conv_kernel = (arguments[i] for i in (0, 2, 9, 10))
        paired_fits = (
            (sizes["grp"], sizes["sp"], sizes["tp"]) == (2, 4, 4)
            and w_query.shape[1] == 2 * head_gain.shape[0]
            and w_query.shape[0] % 32 == 0
            and w_query.shape[0] // 2 <= 3 * head_gain.shape[0]
            and conv_kernel.shape[1] == 2 * head_gain.shape[0]
            and conv_kernel.shape[0] // 2 < 16
        )
        return (paired if paired_fits else on_device)(*arguments)

    placed = (
        P(("grp", "sp"), None),
        P(),
        P("sp", "tp"),
        P("sp", "tp"),
        P("sp", "tp"),
        P("sp", "tp"),
        P("sp", "tp"),
        P("sp", "tp"),
        P(("grp", "sp"), "tp"),
        P(),
        P(None, "tp"),
        P("tp"),
        P("tp"),
        P(None, "tp"),
        P(None, "tp"),
    )
    return jax.shard_map(
        step, mesh=mesh, in_specs=placed, out_specs=P(("grp", "sp"), "tp"), check_vma=False
    )
```
